32 devices in a mesh: ep: 8 (over z, core), tp: 4 (over y, x).
Axes of the slice: x: 2, y: 2, z: 4, core: 2. Of those that a mesh axis runs over, the one named last changes fastest.
Arguments:
- tokens: bfloat16 [1024, 2048], P('ep', 'tp'), may hold values from -6 to 6
- owner_shard: int32 [32768, 1], P('ep'), may hold values from 0 to 7; in each aligned block of 4096 rows (0 to 4095, 4096 to 8191, ...) at most 1024 rows name the same one
- local_row: int32 [32768, 1], P('ep'), may hold values from 0 to 4095
- gate_weights: float32 [1024, 32], P('ep'), may hold values from 0.05 to 1
- up_table: bfloat16 [32768, 2048], P('ep', 'tp'), may hold values from -0.125 to 0.125
- down_table: bfloat16 [32768, 2048], P('ep', 'tp'), may hold values from -6 to 6
Outputs:
- mixed: bfloat16 [1024, 2048], P('ep', 'tp')
The draws below stay inside these ranges and needn't reach their ends.
Inputs may be any that keep to these rules, and one draw needn't show every extreme that they name: `owner_shard`: within the rows of one device (128 tokens of 32 slots each, token by token) no shard is named by more than 1024 slots, a bound that some block reaches; every shard is named somewhere.
All inputs are finite; a program needn't handle non-finite values.
Results may differ from the reference program's by a relative error of at most 0.0049.
Values may be sent and summed in bfloat16 or wider, within the bound.
A program may use at most 128 MiB of HBM per device.

```python
import math
import jax
import jax.numpy as jnp
import numpy as np
from jax import lax

D = 2048
EXP_DEV = 4096
SLOTS = 32
TOK_DEV = 128
EXPERTS = 32768
TOKENS = 1024
CAP = 1024
N_EP = 8


def plant(drawn, rng, low, high):
    longest = drawn.shape.index(max(drawn.shape))
    spots = []
    for shift in (0, 1):
        where = [jax.random.randint(jax.random.fold_in(rng, axis), (), 0, length) for axis, length in enumerate(drawn.shape)]
        where[longest] = (where[longest] + shift) % drawn.shape[longest]
        spots.append(tuple(where))
    return drawn.at[spots[0]].set(low).at[spots[1]].set(high)


def block_levels(key, extent, shards, smallest, largest):
    factor_of, own = 1.0, jax.random.fold_in(key, 6)
    for axis_at, shards_of in shards:
        heights = jnp.exp(jax.random.uniform(jax.random.fold_in(own, axis_at), (shards_of,), jnp.float32, smallest / len(shards), largest / len(shards)))
        factor_of = factor_of * jnp.repeat(heights, extent[axis_at] // shards_of).reshape([-1 if axis == axis_at else 1 for axis in range(len(extent))])
    return factor_of


def rank_table(number_of, slope):
    weights = [(1 << 20) // math.isqrt(standing ** slope) + 1 for standing in range(1, number_of + 1)]
    deviation = 1 + sum(weights) // (1 << 30)
    return np.cumsum(np.array([max(1, weight // deviation) for weight in weights]))


def ranked_ids(key, extent, number_of, slope):
    table = rank_table(number_of, slope)
    pick = jax.random.randint(jax.random.fold_in(key, 1), extent, 0, int(table[number_of - 1]))
    grade = jnp.searchsorted(jnp.asarray(table, jnp.int32), pick, side="right")
    return jax.random.permutation(jax.random.fold_in(key, 2), number_of)[grade].astype(jnp.int32)


def assign_block(key, own, number, rows, number_of, top, reach, skew):
    ranking = jax.random.permutation(key, number_of)
    heavy_load, usual = shares(number_of, rows * top, reach, skew, True), shares(number_of, rows * top, reach, skew, False)
    places = jnp.arange(number_of)

    def named(lengths, turn):
        used = int((lengths > 0).sum())
        fixed = max(1, used // 4)
        moved = fixed + (places - fixed + turn * (used - fixed)) % max(1, number_of - fixed)
        return jnp.zeros((number_of,), jnp.int32).at[ranking[jnp.where(places < fixed, places, moved)]].set(jnp.asarray(lengths, jnp.int32))

    lengths = jnp.where(number % 4 == 0, named(heavy_load, number // 4), named(usual, number - number // 4 - 1))
    mixed = jax.random.permutation(jax.random.fold_in(own, 3), number_of)
    source_of, taker = mixed[0:number_of // 2 * 2:2], mixed[1:number_of // 2 * 2:2]
    room = jnp.minimum(lengths[source_of] - 1, reach - lengths[taker]) // 2
    room = jnp.where((source_of == ranking[0]) | (taker == ranking[0]) | (lengths[taker] == 0), 0, jnp.maximum(room, 0))
    moved = jax.random.randint(jax.random.fold_in(own, 4), (number_of // 2,), 0, 1 << 20) % (room + 1)
    lengths = lengths.at[source_of].add(-moved).at[taker].add(moved)
    items = jnp.searchsorted(jnp.cumsum(lengths), jnp.arange(rows * top), side="right").astype(jnp.int32)
    listing = items.reshape(top, rows).T
    listing = listing[jax.random.permutation(jax.random.fold_in(own, 1), rows)]
    turn = jax.random.randint(jax.random.fold_in(own, 2), (rows, 1), 0, top)
    return jnp.take_along_axis(listing, (jnp.arange(top)[None, :] + turn) % top, axis=1)


def shares(amount, total, limit, lean, full):
    loads = [(1 << 20) // math.isqrt(rank ** lean) + 1 for rank in range(1, amount + 1)]
    largest = limit if full else min(limit, max(-(-total // amount), total * loads[0] // sum(loads)))
    least = 1 if total - largest >= amount - 1 else 0
    holding, rest = [largest] + [least] * (amount - 1), total - largest - least * (amount - 1)
    while rest > 0:
        movable = [i for i in range(1, amount) if holding[i] < largest] or [i for i in range(1, amount) if holding[i] < limit]
        pool, left = sum([loads[i] for i in movable]), rest
        for i in movable:
            extra = min(limit - holding[i], max(1, left * loads[i] // pool), rest)
            holding[i] = holding[i] + extra
            rest = rest - extra
    return np.array(holding)


def scatter_about(key, shape, spread, most, pieces=(), dtype=jnp.bfloat16):
    factor_of = block_levels(key, shape, pieces, -0.22, 0.18) if pieces else 1.0
    result = jax.random.normal(key, shape, jnp.float32) * spread * factor_of
    return jnp.minimum(jnp.maximum(result, -most), most).astype(dtype)


def setup_inputs(seed: int = 0) -> dict:
    splits = jax.random.split(jax.random.key(seed), 7)
    tokens = scatter_about(splits[0], (TOKENS, D), 1.0, 6.0, ((0, 8), (1, 4)))
    owner_shard_keys = jax.random.split(jax.random.fold_in(splits[1], 1), (TOKENS * SLOTS) // (TOK_DEV * SLOTS))
    owner_shard_turns = jax.random.permutation(jax.random.fold_in(splits[1], 3), (TOKENS * SLOTS) // (TOK_DEV * SLOTS))
    owner_shard = jax.vmap(lambda own, number: assign_block(jax.random.fold_in(splits[1], 2), own, number, TOK_DEV * SLOTS, N_EP, 1, CAP, 2))(owner_shard_keys, owner_shard_turns).reshape((TOKENS * SLOTS, 1))
    local_row = plant(ranked_ids(splits[2], (TOKENS * SLOTS, 1), EXP_DEV, 2), jax.random.fold_in(splits[2], 3), 0, EXP_DEV - 1).astype(jnp.int32)
    gate_weights = jnp.clip(jnp.exp(math.log(1.0) - 2.9957323 * jax.random.uniform(splits[3], (TOKENS, SLOTS), jnp.float32) ** block_levels(splits[3], (TOKENS, SLOTS), ((0, 8),), -0.2, 0.2)), 0.05, 1.0)
    up_table = scatter_about(splits[4], (EXPERTS, D), D ** -0.5, 0.125, ((0, 8), (1, 4)))
    down_table = scatter_about(splits[5], (EXPERTS, D), 1.0, 6.0, ((0, 8), (1, 4)))
    return dict(tokens=tokens, owner_shard=owner_shard, local_row=local_row, gate_weights=gate_weights, up_table=up_table, down_table=down_table)


def reference(tokens, owner_shard, local_row, gate_weights, up_table, down_table):
    expert_id = (owner_shard[:, 0] * EXP_DEV + local_row[:, 0]).astype(jnp.int32)
    block_count = TOKENS // TOK_DEV
    id_blocks = expert_id.reshape(block_count, TOK_DEV, SLOTS)
    token_blocks = tokens.reshape(block_count, TOK_DEV, D)
    gate_blocks = gate_weights.reshape(block_count, TOK_DEV, SLOTS)

    def one_block(inputs):
        rows, ids, gates = inputs
        up_rows = up_table[ids].astype(jnp.float32)
        products = jnp.einsum('tsd,td->ts', up_rows, rows.astype(jnp.float32))
        slot_weight = (gates * jax.nn.gelu(products)).astype(jnp.bfloat16)
        down_rows = down_table[ids].astype(jnp.float32)
        summed = jnp.einsum('ts,tsd->td', slot_weight.astype(jnp.float32), down_rows)
        return summed.astype(jnp.bfloat16)

    mixed = lax.map(one_block, (token_blocks, id_blocks, gate_blocks))
    return mixed.reshape(TOKENS, D)
```

```python
import functools

import jax
import jax.numpy as jnp
from jax import lax
from jax.experimental import pallas as pl
from jax.experimental.pallas import tpu as pltpu
from jax.sharding import PartitionSpec as P

MESH = pl.DeviceIdType.MESH
VMEM_BYTES = 60 * 1024 * 1024


def params(number):
    return pltpu.CompilerParams(
        collective_id=number, has_side_effects=True, vmem_limit_bytes=VMEM_BYTES
    )


def vmem():
    return pl.BlockSpec(memory_space=pltpu.VMEM)


def greet(peers):
    barrier = pltpu.get_barrier_semaphore()
    for peer in peers:
        pl.semaphore_signal(barrier, inc=1, device_id=peer, device_id_type=MESH)
    pl.semaphore_wait(barrier, len(peers))


def remote(src, dst, send_sem, recv_sem, peer):
    return pltpu.make_async_remote_copy(
        src_ref=src, dst_ref=dst, send_sem=send_sem, recv_sem=recv_sem,
        device_id=peer, device_id_type=MESH,
    )


def gather_kernel(n_ep, tok_ref, aux_ref, all_tok, all_aux, local_sem, send, recv, fsend, frecv):
    chips = n_ep // 2
    me = lax.axis_index("ep")
    core = lax.rem(me, 2)
    chip = me // 2
    partner = {"ep": me + 1 - 2 * core}

    def at(step):
        return lax.rem(chip + step, chips) * 2 + core

    greet([partner] + [{"ep": at(d)} for d in range(1, chips)])
    pairs = ((tok_ref, all_tok), (aux_ref, all_aux))
    started = []
    for d in range(1, chips):
        for i, (src, dst) in enumerate(pairs):
            copy = remote(src, dst.at[me], send.at[i, d], recv.at[i, d], {"ep": at(d)})
            copy.start()
            started.append(copy)
    local = []
    for i, (src, dst) in enumerate(pairs):
        copy = remote(src, dst.at[me], fsend.at[i, 0], frecv.at[i, 0], partner)
        copy.start()
        started.append(copy)
        own = pltpu.make_async_copy(src, dst.at[me], local_sem.at[i])
        own.start()
        local.append(own)
    for d in range(1, chips):
        source = at(chips - d)
        for i, (src, dst) in enumerate(pairs):
            remote(src, dst.at[source], send.at[i, d], recv.at[i, d], partner).wait_recv()
            copy = remote(dst.at[source], dst.at[source], fsend.at[i, d], frecv.at[i, d], partner)
            copy.start()
            started.append(copy)
    for d in range(chips):
        source = at(chips - d) + 1 - 2 * core
        for i, (src, dst) in enumerate(pairs):
            remote(src, dst.at[source], fsend.at[i, d], frecv.at[i, d], partner).wait_recv()
    for copy in local:
        copy.wait()
    for copy in started:
        copy.wait_send()


def up_kernel(slots, tok_ref, ids_ref, up_hbm, out_ref, up_buf, hi_ref, lo_ref, acc_ref, sems):
    experts, width = up_hbm.shape
    chunks = up_buf.shape[0]
    rows = up_buf.shape[1]
    for c in range(chunks):
        pltpu.make_async_copy(up_hbm.at[pl.ds(c * rows, rows)], up_buf.at[c], sems.at[c]).start()
    blocks = tok_ref.shape[0]
    first = lax.axis_index("ep") * experts
    group = ids_ref.shape[1]
    segments = tok_ref.shape[1] // group
    per_tile = 128 // slots
    lane = lax.broadcasted_iota(jnp.int32, (group, 128), 1) // slots

    def prepare(b, carry):
        for k in range(segments):
            half = k // per_tile
            local = ids_ref[b, :, half * 128:(half + 1) * 128].astype(jnp.int32) - first
            fits = (local >= 0) & (local < experts) & (lane == k % per_tile)
            where = pl.ds(pl.multiple_of((b * segments + k) * group, group), group)
            hi_ref[where, :] = jnp.where(fits, local // 128, -1)
            lo_ref[where, :] = local & 127
        return carry

    lax.fori_loop(0, blocks, prepare, 0)
    acc_ref[...] = jnp.zeros_like(acc_ref)
    tokens = tok_ref.shape[0] * tok_ref.shape[1]

    def step(c, carry):
        pltpu.make_async_copy(up_hbm.at[pl.ds(c * rows, rows)], up_buf.at[c], sems.at[c]).wait()
        product = lax.dot_general(
            tok_ref[...].reshape(tokens, width), up_buf[c], (((1,), (1,)), ((), ())),
            preferred_element_type=jnp.float32,
        )
        acc = acc_ref[...]
        hi = hi_ref[...]
        lo = lo_ref[...]
        for i in range(rows // 128):
            picked = jnp.take_along_axis(
                product[:, i * 128:(i + 1) * 128], lo, axis=1, mode="promise_in_bounds"
            )
            acc = jnp.where(hi == c * (rows // 128) + i, picked, acc)
        acc_ref[...] = acc
        return carry

    lax.fori_loop(0, chunks, step, 0)

    def pack(b, carry):
        halves = []
        for half in range(segments // per_tile):
            total = None
            for k in range(half * per_tile, (half + 1) * per_tile):
                part = acc_ref[pl.ds(pl.multiple_of((b * segments + k) * group, group), group), :]
                total = part if total is None else total + part
            halves.append(total)
        out_ref[pl.ds(pl.multiple_of(b * group, group), group), :] = jnp.concatenate(halves, axis=1)
        return carry

    lax.fori_loop(0, blocks, pack, 0)


def weight_kernel(n_tp, prod_ref, gate_ref, out_ref, got, send, recv, wsend, wrecv):
    me = lax.axis_index("tp")
    rows = prod_ref.shape[0] // n_tp

    def span(q):
        return pl.ds(pl.multiple_of(q * rows, rows), rows)

    def at(step):
        return lax.rem(me + step, n_tp)

    greet([{"tp": at(d)} for d in range(1, n_tp)])
    started = []
    for d in range(1, n_tp):
        copy = remote(prod_ref.at[span(at(d))], got.at[d - 1], send.at[d], recv.at[d], {"tp": at(d)})
        copy.start()
        started.append(copy)
    total = prod_ref[span(me), :]
    for d, copy in enumerate(started):
        copy.wait_recv()
        total += got[d]
    out_ref[span(me), :] = (gate_ref[span(me), :] * jax.nn.gelu(total)).astype(jnp.bfloat16)
    for d in range(1, n_tp):
        copy = remote(out_ref.at[span(me)], out_ref.at[span(me)], wsend.at[d], wrecv.at[d], {"tp": at(d)})
        copy.start()
        started.append(copy)
    for d in range(1, n_tp):
        source = span(at(n_tp - d))
        remote(out_ref.at[source], out_ref.at[source], wsend.at[d], wrecv.at[d], {"tp": at(d)}).wait_recv()
    for copy in started:
        copy.wait_send()


def down_kernel(n_ep, slots, wts_ref, ids_ref, down_hbm, out_ref, down_buf, w_ref, own, xbuf, ybuf,
                sbuf, rbuf, dsem, xsend, xrecv, send, recv):
    chips = n_ep // 2
    me = lax.axis_index("ep")
    core = lax.rem(me, 2)
    chip = me // 2
    partner = {"ep": me + 1 - 2 * core}
    load = pltpu.make_async_copy(down_hbm, down_buf, dsem)
    load.start()

    def at(step):
        return lax.rem(chip + step, chips)

    greet([partner] + [{"ep": at(d) * 2 + core} for d in range(1, chips)])
    experts = down_hbm.shape[0]
    tiles = experts // 128
    first = me * experts
    group = ids_ref.shape[1]
    lanes = ids_ref.shape[2]
    tokens = lanes // slots
    block = group * tokens
    row_key = lax.broadcasted_iota(jnp.int32, (tiles * tokens, lanes), 0)
    low_key = lax.broadcasted_iota(jnp.int32, (128, lanes), 0)
    turn = lax.broadcasted_iota(jnp.int32, (1, lanes), 1) // slots

    def spread(b, j):
        local = ids_ref[b, pl.ds(j, 1), :].astype(jnp.int32) - first
        weight = wts_ref[b, pl.ds(j, 1), :]
        fits = (local >= 0) & (local < experts)
        key = jnp.where(fits, (local // 128) * tokens + turn, -1)
        left = jnp.where(row_key == key, weight, 0.0).astype(jnp.bfloat16)
        right = jnp.where(low_key == (local & 127), 1.0, 0.0).astype(jnp.bfloat16)
        wide = lax.dot_general(left, right, (((1,), (1,)), ((), ())), preferred_element_type=jnp.float32)
        return wide.reshape(tiles, tokens, 128)

    loaded = False
    copies = []

    def finish(i):
        d = i + 1
        copies[i].wait_recv()
        sbuf[i] = (own[i] + ybuf[i].astype(jnp.float32)).astype(jnp.bfloat16)
        copy = remote(sbuf.at[i], rbuf.at[i], send.at[i], recv.at[i], {"ep": at(d) * 2 + core})
        copy.start()
        return copy

    sent = []
    for i in range(chips):
        target = at(i + 1)

        def build(x, carry):
            b = target * 2 + x // (group // 2)
            j = lax.rem(x, group // 2) * 2
            both = jnp.concatenate([spread(b, j), spread(b, j + 1)], axis=1).astype(jnp.bfloat16)
            for h in range(tiles):
                w_ref[pl.ds(pl.multiple_of(x * 16, 16), 16), h * 128:(h + 1) * 128] = both[h]
            return carry

        lax.fori_loop(0, group, build, 0)
        if not loaded:
            load.wait()
            loaded = True
        part = jnp.dot(w_ref[...], down_buf[...], preferred_element_type=jnp.float32)
        low, high = part[:block], part[block:]
        mine = jnp.where(core == 0, low, high)
        other = jnp.where(core == 0, high, low)
        own[i] = mine
        xbuf[i] = other.astype(jnp.bfloat16)
        copy = remote(xbuf.at[i], ybuf.at[i], xsend.at[i], xrecv.at[i], partner)
        copy.start()
        copies.append(copy)
        if i > 0:
            sent.append(finish(i - 1))
    last = chips - 1
    copies[last].wait_recv()
    total = own[last] + ybuf[last].astype(jnp.float32)
    for i, copy in enumerate(sent):
        copy.wait_recv()
        total += rbuf[i].astype(jnp.float32)
    out_ref[...] = total.astype(jnp.bfloat16)
    for copy in copies + sent:
        copy.wait_send()


def on_device(tokens, owner_shard, local_row, gate_weights, up_table, down_table):
    n_ep, n_tp = lax.axis_size("ep"), lax.axis_size("tp")
    count, width = tokens.shape
    slots = gate_weights.shape[1]
    experts = up_table.shape[0]
    side = 8
    group, lanes = count // side, side * slots
    chips = n_ep // 2
    shuffled = tokens.reshape(group, side, width).transpose(1, 0, 2).reshape(count, width)
    ids = owner_shard[:, 0] * experts + local_row[:, 0]
    aux = jnp.stack([ids.astype(jnp.float32).reshape(group, lanes), gate_weights.reshape(group, lanes)])
    dma = pltpu.SemaphoreType.DMA
    all_tok, all_aux = pl.pallas_call(
        functools.partial(gather_kernel, n_ep),
        out_shape=(
            jax.ShapeDtypeStruct((n_ep, count, width), jnp.bfloat16),
            jax.ShapeDtypeStruct((n_ep, 2, group, lanes), jnp.float32),
        ),
        in_specs=[vmem()] * 2,
        out_specs=(vmem(), vmem()),
        scratch_shapes=[dma((2,)), dma((2, chips)), dma((2, chips)), dma((2, chips)), dma((2, chips))],
        compiler_params=params(0),
        name="gather_tokens",
    )(shuffled, aux)
    all_ids = all_aux[:, 0]
    gates = all_aux[:, 1].reshape(n_ep * group, lanes)
    total = n_ep * count
    chunks = 16
    products = pl.pallas_call(
        functools.partial(up_kernel, slots),
        out_shape=jax.ShapeDtypeStruct((n_ep * group, lanes), jnp.float32),
        in_specs=[vmem(), vmem(), pl.BlockSpec(memory_space=pl.ANY)],
        out_specs=vmem(),
        scratch_shapes=[
            pltpu.VMEM((chunks, experts // chunks, width), jnp.bfloat16),
            pltpu.VMEM((total, 128), jnp.int32),
            pltpu.VMEM((total, 128), jnp.int32),
            pltpu.VMEM((total, 128), jnp.float32),
            dma((chunks,)),
        ],
        compiler_params=pltpu.CompilerParams(vmem_limit_bytes=VMEM_BYTES),
        name="up_products",
    )(all_tok, all_ids, up_table)
    weights = pl.pallas_call(
        functools.partial(weight_kernel, n_tp),
        out_shape=jax.ShapeDtypeStruct((n_ep * group, lanes), jnp.bfloat16),
        in_specs=[vmem()] * 2,
        out_specs=vmem(),
        scratch_shapes=[
            pltpu.VMEM((n_tp - 1, n_ep * group // n_tp, lanes), jnp.float32),
            dma((n_tp,)), dma((n_tp,)), dma((n_tp,)), dma((n_tp,)),
        ],
        compiler_params=params(1),
        name="slot_weights",
    )(products, gates)
    weights = weights.astype(jnp.float32).reshape(n_ep, group, lanes)
    return pl.pallas_call(
        functools.partial(down_kernel, n_ep, slots),
        out_shape=jax.ShapeDtypeStruct((count, width), jnp.bfloat16),
        in_specs=[vmem(), vmem(), pl.BlockSpec(memory_space=pl.ANY)],
        out_specs=vmem(),
        scratch_shapes=[
            pltpu.VMEM((experts, width), jnp.bfloat16),
            pltpu.VMEM((2 * count, experts), jnp.bfloat16),
            pltpu.VMEM((chips, count, width), jnp.float32),
            pltpu.VMEM((chips, count, width), jnp.bfloat16),
            pltpu.VMEM((chips, count, width), jnp.bfloat16),
            pltpu.VMEM((chips, count, width), jnp.bfloat16),
            pltpu.VMEM((chips, count, width), jnp.bfloat16),
            dma, dma((chips,)), dma((chips,)), dma((chips,)), dma((chips,)),
        ],
        compiler_params=params(2),
        name="down_sums",
    )(weights, all_ids, down_table)


def solution(mesh):
    return jax.shard_map(
        on_device,
        mesh=mesh,
        in_specs=(
            P("ep", "tp"),
            P("ep", None),
            P("ep", None),
            P("ep", None),
            P("ep", "tp"),
            P("ep", "tp"),
        ),
        out_specs=P("ep", "tp"),
        check_vma=False,
    )
```

```python
import functools

import jax
import jax.numpy as jnp
from jax import lax
from jax.experimental import pallas as pl
from jax.experimental.pallas import tpu as pltpu
from jax.sharding import PartitionSpec as P

MESH = pl.DeviceIdType.MESH
VMEM_BYTES = 60 * 1024 * 1024


def params(number):
    return pltpu.CompilerParams(
        collective_id=number, has_side_effects=True, vmem_limit_bytes=VMEM_BYTES
    )


def vmem():
    return pl.BlockSpec(memory_space=pltpu.VMEM)


def greet(peers):
    barrier = pltpu.get_barrier_semaphore()
    for peer in peers:
        pl.semaphore_signal(barrier, inc=1, device_id=peer, device_id_type=MESH)
    pl.semaphore_wait(barrier, len(peers))


def remote(src, dst, send_sem, recv_sem, peer):
    return pltpu.make_async_remote_copy(
        src_ref=src, dst_ref=dst, send_sem=send_sem, recv_sem=recv_sem,
        device_id=peer, device_id_type=MESH,
    )


def fused_kernel(n_ep, n_tp, slots, tok_ref, aux_ref, up_hbm, down_hbm, out_ref,
                 all_tok, all_aux, up_buf, down_buf, hi_ref, lo_ref, acc_ref, pbuf, pgot, wt_ref, w_ref,
                 own, xbuf, ybuf, sbuf, rbuf,
                 local_sem, send, recv, fsend, frecv, up_sem, down_sem, psend, precv,
                 xsend, xrecv, rsend, rrecv):
    chips = n_ep // 2
    me = lax.axis_index("ep")
    core = lax.rem(me, 2)
    chip = me // 2
    part = lax.axis_index("tp")
    partner = {"ep": me + 1 - 2 * core}
    experts, width = up_hbm.shape
    chunks, chunk_rows = up_buf.shape[0], up_buf.shape[1]
    tiles = experts // 128
    first = me * experts
    group, lanes = aux_ref.shape[1], aux_ref.shape[2]
    side = lanes // slots
    block = group * side
    per_tile = 128 // slots

    def at(step):
        return lax.rem(chip + step, chips)

    def counterpart(step):
        return {"ep": at(step) * 2 + core}

    def tp_peer(step):
        return {"tp": lax.rem(part + step, n_tp)}

    up_loads = []
    for c in range(chunks):
        load = pltpu.make_async_copy(up_hbm.at[pl.ds(c * chunk_rows, chunk_rows)], up_buf.at[c], up_sem.at[c])
        load.start()
        up_loads.append(load)
    greet([partner] + [counterpart(d) for d in range(1, chips)] + [tp_peer(d) for d in range(1, n_tp)])

    pairs = ((aux_ref, all_aux), (tok_ref, all_tok))
    started = []
    local = []
    for i, (src, dst) in enumerate(pairs):
        own_copy = pltpu.make_async_copy(src, dst.at[me], local_sem.at[i])
        own_copy.start()
        local.append(own_copy)
        copy = remote(src, dst.at[me], fsend.at[i, 0], frecv.at[i, 0], partner)
        copy.start()
        started.append(copy)
    for d in range(1, chips):
        for i, (src, dst) in enumerate(pairs):
            copy = remote(src, dst.at[me], send.at[i, d], recv.at[i, d], counterpart(d))
            copy.start()
            started.append(copy)
    down_load = pltpu.make_async_copy(down_hbm, down_buf, down_sem)
    down_load.start()

    def forward(d):
        source = at(chips - d) * 2 + core
        for i, (src, dst) in enumerate(pairs):
            remote(src, dst.at[source], send.at[i, d], recv.at[i, d], partner).wait_recv()
            copy = remote(dst.at[source], dst.at[source], fsend.at[i, d], frecv.at[i, d], partner)
            copy.start()
            started.append(copy)

    def arrive(d):
        source = at(chips - d) * 2 + 1 - core
        for i, (src, dst) in enumerate(pairs):
            remote(src, dst.at[source], fsend.at[i, d], frecv.at[i, d], partner).wait_recv()

    lane = lax.broadcasted_iota(jnp.int32, (group, 128), 1) // slots

    def up_step(d, base):
        for b in range(2):
            for k in range(side):
                half = k // per_tile
                here = all_aux[base + b, 0, :, half * 128:(half + 1) * 128].astype(jnp.int32) - first
                fits = (here >= 0) & (here < experts) & (lane == k % per_tile)
                where = pl.ds(b * block + k, group, stride=side)
                hi_ref[where, :] = jnp.where(fits, here // 128, -1)
                lo_ref[where, :] = here & 127
        acc_ref[...] = jnp.zeros_like(acc_ref)
        if d == 0:
            for load in up_loads:
                load.wait()

        def chunk(c, carry):
            product = lax.dot_general(
                all_tok[pl.ds(base, 2)].reshape(2 * block, width), up_buf[c], (((1,), (1,)), ((), ())),
                preferred_element_type=jnp.float32,
            )
            acc = acc_ref[...]
            hi = hi_ref[...]
            lo = lo_ref[...]
            for i in range(chunk_rows // 128):
                picked = jnp.take_along_axis(
                    product[:, i * 128:(i + 1) * 128], lo, axis=1, mode="promise_in_bounds"
                )
                acc = jnp.where(hi == c * (chunk_rows // 128) + i, picked, acc)
            acc_ref[...] = acc
            return carry

        lax.fori_loop(0, chunks, chunk, 0)
        for b in range(2):
            for half in range(side // per_tile):
                total = None
                for k in range(half * per_tile, (half + 1) * per_tile):
                    piece = acc_ref[pl.ds(b * block + k, group, stride=side), :]
                    total = piece if total is None else total + piece
                pbuf[d, b, :, half * 128:(half + 1) * 128] = total
        copies = []
        for t in range(1, n_tp):
            copy = remote(pbuf.at[d], pgot.at[d, t], psend.at[d, t], precv.at[d, t], tp_peer(t))
            copy.start()
            copies.append(copy)
        started.extend(copies)
        return copies

    row_key = lax.broadcasted_iota(jnp.int32, (tiles * side, lanes), 0)
    low_key = lax.broadcasted_iota(jnp.int32, (128, lanes), 0)
    turn = lax.broadcasted_iota(jnp.int32, (1, lanes), 1) // slots

    def down_step(d, base, copies):
        total = pbuf[d]
        for t, copy in enumerate(copies):
            copy.wait_recv()
            total += pgot[d, t + 1]
        gate = all_aux[pl.ds(base, 2), 1]
        wt_ref[...] = (gate * jax.nn.gelu(total)).astype(jnp.bfloat16).astype(jnp.float32)

        def spread(b, j):
            here = all_aux[base + b, 0, pl.ds(j, 1), :].astype(jnp.int32) - first
            weight = wt_ref[b, pl.ds(j, 1), :]
            fits = (here >= 0) & (here < experts)
            key = jnp.where(fits, (here // 128) * side + turn, -1)
            left = jnp.where(row_key == key, weight, 0.0).astype(jnp.bfloat16)
            right = jnp.where(low_key == (here & 127), 1.0, 0.0).astype(jnp.bfloat16)
            wide = lax.dot_general(left, right, (((1,), (1,)), ((), ())), preferred_element_type=jnp.float32)
            return wide.reshape(tiles, side, 128)

        def build(x, carry):
            b = x // (group // 2)
            j = lax.rem(x, group // 2) * 2
            both = jnp.concatenate([spread(b, j), spread(b, j + 1)], axis=1).astype(jnp.bfloat16)
            for h in range(tiles):
                w_ref[pl.ds(pl.multiple_of(x * 2 * side, 2 * side), 2 * side), h * 128:(h + 1) * 128] = both[h]
            return carry

        lax.fori_loop(0, group, build, 0)
        if d == 0:
            down_load.wait()
        sums = jnp.dot(w_ref[...], down_buf[...], preferred_element_type=jnp.float32)
        low, high = sums[:block], sums[block:]
        own[d] = jnp.where(core == 0, low, high)
        xbuf[d] = jnp.where(core == 0, high, low).astype(jnp.bfloat16)
        copy = remote(xbuf.at[d], ybuf.at[d], xsend.at[d], xrecv.at[d], partner)
        copy.start()
        started.append(copy)
        return copy

    returned = []

    def finish(d, copy):
        copy.wait_recv()
        if d == 0:
            return
        sbuf[d] = (own[d] + ybuf[d].astype(jnp.float32)).astype(jnp.bfloat16)
        copy = remote(sbuf.at[d], rbuf.at[d], rsend.at[d], rrecv.at[d], counterpart(chips - d))
        copy.start()
        returned.append(copy)

    def base_of(d):
        return at(chips - d) * 2 if d else chip * 2

    for copy in local:
        copy.wait()
    waiting = None
    exchanged = None
    for d in range(chips + 1):
        if d < chips:
            arrive(d)
            sending = up_step(d, base_of(d))
            if d + 1 < chips:
                forward(d + 1)
        else:
            sending = None
        if d > 0:
            copy = down_step(d - 1, base_of(d - 1), waiting)
            if exchanged is not None:
                finish(d - 2, exchanged)
            exchanged = copy
        waiting = sending
    finish(chips - 1, exchanged)
    total = own[0] + ybuf[0].astype(jnp.float32)
    for d, copy in enumerate(returned):
        copy.wait_recv()
        total += rbuf[d + 1].astype(jnp.float32)
    out_ref[...] = total.astype(jnp.bfloat16)
    for copy in started + returned:
        copy.wait_send()


def on_device(tokens, owner_shard, local_row, gate_weights, up_table, down_table):
    n_ep, n_tp = lax.axis_size("ep"), lax.axis_size("tp")
    count, width = tokens.shape
    slots = gate_weights.shape[1]
    experts = up_table.shape[0]
    side = 8
    group, lanes = count // side, side * slots
    chips = n_ep // 2
    ids = owner_shard[:, 0] * experts + local_row[:, 0]
    aux = jnp.stack([ids.astype(jnp.float32).reshape(group, lanes), gate_weights.reshape(group, lanes)])
    dma = pltpu.SemaphoreType.DMA
    chunks = experts // 512
    wide = (chips, count, width)
    anywhere = pl.BlockSpec(memory_space=pl.ANY)
    return pl.pallas_call(
        functools.partial(fused_kernel, n_ep, n_tp, slots),
        out_shape=jax.ShapeDtypeStruct((count, width), jnp.bfloat16),
        in_specs=[vmem(), vmem(), anywhere, anywhere],
        out_specs=vmem(),
        scratch_shapes=[
            pltpu.VMEM((n_ep, count, width), jnp.bfloat16),
            pltpu.VMEM((n_ep, 2, group, lanes), jnp.float32),
            pltpu.VMEM((chunks, experts // chunks, width), jnp.bfloat16),
            pltpu.VMEM((experts, width), jnp.bfloat16),
            pltpu.VMEM((2 * count, 128), jnp.int32),
            pltpu.VMEM((2 * count, 128), jnp.int32),
            pltpu.VMEM((2 * count, 128), jnp.float32),
            pltpu.VMEM((chips, 2, group, lanes), jnp.float32),
            pltpu.VMEM((chips, n_tp, 2, group, lanes), jnp.float32),
            pltpu.VMEM((2, group, lanes), jnp.float32),
            pltpu.VMEM((2 * count, experts), jnp.bfloat16),
            pltpu.VMEM(wide, jnp.float32),
            pltpu.VMEM(wide, jnp.bfloat16),
            pltpu.VMEM(wide, jnp.bfloat16),
            pltpu.VMEM(wide, jnp.bfloat16),
            pltpu.VMEM(wide, jnp.bfloat16),
            dma((2,)), dma((2, chips)), dma((2, chips)), dma((2, chips)), dma((2, chips)),
            dma((chunks,)), dma, dma((chips, n_tp)), dma((chips, n_tp)),
            dma((chips,)), dma((chips,)), dma((chips,)), dma((chips,)),
        ],
        compiler_params=params(0),
        name="retrieve",
    )(tokens, aux, up_table, down_table)


def solution(mesh):
    return jax.shard_map(
        on_device,
        mesh=mesh,
        in_specs=(
            P("ep", "tp"),
            P("ep", None),
            P("ep", None),
            P("ep", None),
            P("ep", "tp"),
            P("ep", "tp"),
        ),
        out_specs=P("ep", "tp"),
        check_vma=False,
    )
```

```python
import functools

import jax
import jax.numpy as jnp
from jax import lax
from jax.experimental import pallas as pl
from jax.experimental.pallas import tpu as pltpu
from jax.sharding import PartitionSpec as P

MESH = pl.DeviceIdType.MESH
VMEM_BYTES = 60 * 1024 * 1024


def params(number):
    return pltpu.CompilerParams(
        collective_id=number, has_side_effects=True, vmem_limit_bytes=VMEM_BYTES
    )


def vmem():
    return pl.BlockSpec(memory_space=pltpu.VMEM)


def greet(peers):
    barrier = pltpu.get_barrier_semaphore()
    for peer in peers:
        pl.semaphore_signal(barrier, inc=1, device_id=peer, device_id_type=MESH)
    pl.semaphore_wait(barrier, len(peers))


def remote(src, dst, send_sem, recv_sem, peer):
    return pltpu.make_async_remote_copy(
        src_ref=src, dst_ref=dst, send_sem=send_sem, recv_sem=recv_sem,
        device_id=peer, device_id_type=MESH,
    )


def fused_kernel(n_ep, n_tp, slots, tok_ref, aux_ref, up_hbm, down_hbm, out_ref,
                 all_tok, all_aux, up_buf, down_buf, hi_ref, lo_ref, acc_ref, pbuf, pgot, wt_ref, w_ref,
                 own, xbuf, ybuf, sbuf, rbuf,
                 local_sem, send, recv, fsend, frecv, up_sem, down_sem, psend, precv,
                 xsend, xrecv, rsend, rrecv):
    chips = n_ep // 2
    me = lax.axis_index("ep")
    core = lax.rem(me, 2)
    chip = me // 2
    part = lax.axis_index("tp")
    partner = {"ep": me + 1 - 2 * core}
    experts, width = up_hbm.shape
    chunks, chunk_rows = up_buf.shape[0], up_buf.shape[1]
    tiles = experts // 128
    first = me * experts
    group, lanes = aux_ref.shape[1], aux_ref.shape[2]
    side = lanes // slots
    block = group * side
    per_tile = 128 // slots

    def at(step):
        return lax.rem(chip + step, chips)

    def counterpart(step):
        return {"ep": at(step) * 2 + core}

    def tp_peer(step):
        return {"tp": lax.rem(part + step, n_tp)}

    up_loads = []
    for c in range(chunks):
        load = pltpu.make_async_copy(up_hbm.at[pl.ds(c * chunk_rows, chunk_rows)], up_buf.at[c], up_sem.at[c])
        load.start()
        up_loads.append(load)
    greet([partner] + [counterpart(d) for d in range(1, chips)] + [tp_peer(d) for d in range(1, n_tp)])

    pairs = ((aux_ref, all_aux), (tok_ref, all_tok))
    started = []
    local = []
    for i, (src, dst) in enumerate(pairs):
        own_copy = pltpu.make_async_copy(src, dst.at[me], local_sem.at[i])
        own_copy.start()
        local.append(own_copy)
        copy = remote(src, dst.at[me], fsend.at[i, 0], frecv.at[i, 0], partner)
        copy.start()
        started.append(copy)
    for d in range(1, chips):
        for i, (src, dst) in enumerate(pairs):
            copy = remote(src, dst.at[me], send.at[i, d], recv.at[i, d], counterpart(d))
            copy.start()
            started.append(copy)
    down_load = pltpu.make_async_copy(down_hbm, down_buf, down_sem)
    down_load.start()

    def forward(d):
        source = at(chips - d) * 2 + core
        for i, (src, dst) in enumerate(pairs):
            remote(src, dst.at[source], send.at[i, d], recv.at[i, d], partner).wait_recv()
            copy = remote(dst.at[source], dst.at[source], fsend.at[i, d], frecv.at[i, d], partner)
            copy.start()
            started.append(copy)

    def arrive(d):
        source = at(chips - d) * 2 + 1 - core
        for i, (src, dst) in enumerate(pairs):
            remote(src, dst.at[source], fsend.at[i, d], frecv.at[i, d], partner).wait_recv()

    lane = lax.broadcasted_iota(jnp.int32, (group, 128), 1) // slots

    def up_step(d, base):
        for b in range(2):
            for k in range(side):
                half = k // per_tile
                here = all_aux[base + b, 0, :, half * 128:(half + 1) * 128].astype(jnp.int32) - first
                fits = (here >= 0) & (here < experts) & (lane == k % per_tile)
                where = pl.ds(b * block + k, group, stride=side)
                hi_ref[where, :] = jnp.where(fits, here // 128, -1)
                lo_ref[where, :] = here & 127
        acc_ref[...] = jnp.zeros_like(acc_ref)
        if d == 0:
            for load in up_loads:
                load.wait()

        def chunk(c, carry):
            product = lax.dot_general(
                all_tok[pl.ds(base, 2)].reshape(2 * block, width), up_buf[c], (((1,), (1,)), ((), ())),
                preferred_element_type=jnp.float32,
            )
            acc = acc_ref[...]
            hi = hi_ref[...]
            lo = lo_ref[...]
            for i in range(chunk_rows // 128):
                picked = jnp.take_along_axis(
                    product[:, i * 128:(i + 1) * 128], lo, axis=1, mode="promise_in_bounds"
                )
                acc = jnp.where(hi == c * (chunk_rows // 128) + i, picked, acc)
            acc_ref[...] = acc
            return carry

        lax.fori_loop(0, chunks, chunk, 0, unroll=4)
        for b in range(2):
            for half in range(side // per_tile):
                total = None
                for k in range(half * per_tile, (half + 1) * per_tile):
                    piece = acc_ref[pl.ds(b * block + k, group, stride=side), :]
                    total = piece if total is None else total + piece
                pbuf[d, b, :, half * 128:(half + 1) * 128] = total
        copies = []
        for t in range(1, n_tp):
            copy = remote(pbuf.at[d], pgot.at[d, t], psend.at[d, t], precv.at[d, t], tp_peer(t))
            copy.start()
            copies.append(copy)
        started.extend(copies)
        return copies

    def row_keys(count):
        keys = lax.broadcasted_iota(jnp.int32, (count, lanes), 0).astype(jnp.float32)
        return keys.astype(jnp.bfloat16).reshape(count // 16, 16, lanes)

    row_key = row_keys(tiles * side)
    low_key = row_keys(128)
    turn = lax.broadcasted_iota(jnp.int32, (16, lanes), 1) // slots
    zero = jnp.zeros((1, 16, lanes), jnp.bfloat16)
    one = jnp.ones((1, 16, lanes), jnp.bfloat16)

    def narrow(x):
        return x.astype(jnp.float32).astype(jnp.bfloat16)[None]

    def down_step(d, base, copies):
        total = pbuf[d]
        for t, copy in enumerate(copies):
            copy.wait_recv()
            total += pgot[d, t + 1]
        gate = all_aux[pl.ds(base, 2), 1]
        wt_ref[...] = (gate * jax.nn.gelu(total)).astype(jnp.bfloat16).astype(jnp.float32)

        def spread(b, j):
            here = jnp.broadcast_to(all_aux[base + b, 0, pl.ds(j, 1), :], (16, lanes)).astype(jnp.int32) - first
            weight = jnp.broadcast_to(wt_ref[b, pl.ds(j, 1), :], (16, lanes)).astype(jnp.bfloat16)[None]
            fits = (here >= 0) & (here < experts)
            key = narrow(jnp.where(fits, (here // 128) * side + turn, -1))
            left = jnp.where(row_key == key, weight, zero).reshape(tiles * side, lanes)
            right = jnp.where(low_key == narrow(here & 127), one, zero).reshape(128, lanes)
            wide = lax.dot_general(left, right, (((1,), (1,)), ((), ())), preferred_element_type=jnp.float32)
            return wide.reshape(tiles, side, 128)

        def build(x, carry):
            b = x // (group // 2)
            j = lax.rem(x, group // 2) * 2
            both = jnp.concatenate([spread(b, j), spread(b, j + 1)], axis=1).astype(jnp.bfloat16)
            for h in range(tiles):
                w_ref[pl.ds(pl.multiple_of(x * 2 * side, 2 * side), 2 * side), h * 128:(h + 1) * 128] = both[h]
            return carry

        lax.fori_loop(0, group, build, 0, unroll=4)
        if d == 0:
            down_load.wait()
        sums = jnp.dot(w_ref[...], down_buf[...], preferred_element_type=jnp.float32)
        low, high = sums[:block], sums[block:]
        own[d] = jnp.where(core == 0, low, high)
        xbuf[d] = jnp.where(core == 0, high, low).astype(jnp.bfloat16)
        copy = remote(xbuf.at[d], ybuf.at[d], xsend.at[d], xrecv.at[d], partner)
        copy.start()
        started.append(copy)
        return copy

    returned = []

    def finish(d, copy):
        copy.wait_recv()
        if d == 0:
            return
        sbuf[d] = (own[d] + ybuf[d].astype(jnp.float32)).astype(jnp.bfloat16)
        copy = remote(sbuf.at[d], rbuf.at[d], rsend.at[d], rrecv.at[d], counterpart(chips - d))
        copy.start()
        returned.append(copy)

    def base_of(d):
        return at(chips - d) * 2 if d else chip * 2

    for copy in local:
        copy.wait()
    waiting = None
    exchanged = None
    for d in range(chips + 1):
        if d < chips:
            arrive(d)
            sending = up_step(d, base_of(d))
            if d + 1 < chips:
                forward(d + 1)
        else:
            sending = None
        if d > 0:
            copy = down_step(d - 1, base_of(d - 1), waiting)
            if exchanged is not None:
                finish(d - 2, exchanged)
            exchanged = copy
        waiting = sending
    finish(chips - 1, exchanged)
    total = own[0] + ybuf[0].astype(jnp.float32)
    for d, copy in enumerate(returned):
        copy.wait_recv()
        total += rbuf[d + 1].astype(jnp.float32)
    out_ref[...] = total.astype(jnp.bfloat16)
    for copy in started + returned:
        copy.wait_send()


def on_device(tokens, owner_shard, local_row, gate_weights, up_table, down_table):
    n_ep, n_tp = lax.axis_size("ep"), lax.axis_size("tp")
    count, width = tokens.shape
    slots = gate_weights.shape[1]
    experts = up_table.shape[0]
    side = 8
    group, lanes = count // side, side * slots
    chips = n_ep // 2
    ids = owner_shard[:, 0] * experts + local_row[:, 0]
    aux = jnp.stack([ids.astype(jnp.float32).reshape(group, lanes), gate_weights.reshape(group, lanes)])
    dma = pltpu.SemaphoreType.DMA
    chunks = experts // 512
    wide = (chips, count, width)
    anywhere = pl.BlockSpec(memory_space=pl.ANY)
    return pl.pallas_call(
        functools.partial(fused_kernel, n_ep, n_tp, slots),
        out_shape=jax.ShapeDtypeStruct((count, width), jnp.bfloat16),
        in_specs=[vmem(), vmem(), anywhere, anywhere],
        out_specs=vmem(),
        scratch_shapes=[
            pltpu.VMEM((n_ep, count, width), jnp.bfloat16),
            pltpu.VMEM((n_ep, 2, group, lanes), jnp.float32),
            pltpu.VMEM((chunks, experts // chunks, width), jnp.bfloat16),
            pltpu.VMEM((experts, width), jnp.bfloat16),
            pltpu.VMEM((2 * count, 128), jnp.int32),
            pltpu.VMEM((2 * count, 128), jnp.int32),
            pltpu.VMEM((2 * count, 128), jnp.float32),
            pltpu.VMEM((chips, 2, group, lanes), jnp.float32),
            pltpu.VMEM((chips, n_tp, 2, group, lanes), jnp.float32),
            pltpu.VMEM((2, group, lanes), jnp.float32),
            pltpu.VMEM((2 * count, experts), jnp.bfloat16),
            pltpu.VMEM(wide, jnp.float32),
            pltpu.VMEM(wide, jnp.bfloat16),
            pltpu.VMEM(wide, jnp.bfloat16),
            pltpu.VMEM(wide, jnp.bfloat16),
            pltpu.VMEM(wide, jnp.bfloat16),
            dma((2,)), dma((2, chips)), dma((2, chips)), dma((2, chips)), dma((2, chips)),
            dma((chunks,)), dma, dma((chips, n_tp)), dma((chips, n_tp)),
            dma((chips,)), dma((chips,)), dma((chips,)), dma((chips,)),
        ],
        compiler_params=params(0),
        name="retrieve",
    )(tokens, aux, up_table, down_table)


def solution(mesh):
    return jax.shard_map(
        on_device,
        mesh=mesh,
        in_specs=(
            P("ep", "tp"),
            P("ep", None),
            P("ep", None),
            P("ep", None),
            P("ep", "tp"),
            P("ep", "tp"),
        ),
        out_specs=P("ep", "tp"),
        check_vma=False,
    )
```
